32 devices in a mesh: sp: 16 (over z, y, x), tp: 2 (over core).
Axes of the slice: x: 2, y: 2, z: 4, core: 2. Of those that a mesh axis runs over, the one named last changes fastest.
Arguments:
- tokens: bfloat16 [8192, 3072], P('sp'), may hold values from -72 to 72
- w_query: bfloat16 [3072, 1024], P('sp', 'tp'), may hold values from -0.109375 to 0.109375
- w_key: bfloat16 [3072, 1024], P('sp', 'tp'), may hold values from -0.109375 to 0.109375
- w_value: bfloat16 [3072, 1024], P('sp', 'tp'), may hold values from -0.4375 to 0.4375
- w_out: bfloat16 [1024, 3072], P('tp', 'sp'), may hold values from -0.1875 to 0.1875
Outputs:
- mixed: bfloat16 [8192, 3072], P(('sp', 'tp'))
- row_lse: float32 [16, 8192], P('tp', 'sp')
The draws below stay inside these ranges and needn't reach their ends.
All inputs are finite; a program needn't handle non-finite values.
Results may differ from the reference program's by a relative error of at most 0.014.
Values may be sent and summed in bfloat16 or wider, within the bound.
No kernel may reach another device: no remote copies, remote signals or barrier semaphores. Data moves between devices by JAX's collectives and lax.ppermute only.
A program may use at most 64 MiB of HBM per device.

```python
import jax
import jax.numpy as jnp
from jax import lax

D = 3072
HEADS = 16
HEAD_SIZE = 64
KEYS_BEHIND = 128
D_ATT = 1024
SEQUENCE_TOKENS = 8192
N_TP = 2


def draw_tokens(key, part):
    base_offset = jax.random.truncated_normal(key, -6.0, 6.0, (SEQUENCE_TOKENS, D), jnp.float32)
    return base_offset.astype(jnp.bfloat16)


def block_levels(own_key, extent, pieces, least, high):
    factor_of = 1.0
    for dim, blocks in pieces:
        steps = jax.random.uniform(jax.random.fold_in(jax.random.fold_in(own_key, 6), dim), (blocks,), jnp.float32, least / len(pieces), high / len(pieces))
        factor_of = factor_of * jnp.repeat(jnp.exp(steps), extent[dim] // blocks).reshape((-1,) + (1,) * (len(extent) - 1 - dim))
    return factor_of


def centred(key, extent, spread, bound, pieces=(), held_as=jnp.bfloat16):
    result = jax.random.normal(key, extent, jnp.float32) * spread
    if len(pieces) > 0:
        result = block_levels(key, extent, pieces, -0.22, 0.18) * result
    return jnp.clip(result, min=-bound, max=bound).astype(held_as)


def setup_inputs(seed: int = 0) -> dict:
    arg_keys = jax.random.split(jax.random.key(seed), 6)
    tokens = draw_tokens(jax.random.fold_in(arg_keys[5], 71), 0)
    w_query = centred(arg_keys[1], (D, D_ATT), D ** -0.5, 0.109375, ((0, 16), (1, 2)))
    w_key = centred(arg_keys[2], (D, D_ATT), D ** -0.5, 0.109375, ((0, 16), (1, 2)))
    w_value = centred(arg_keys[3], (D, D_ATT), (D // 16) ** -0.5, 0.4375, ((0, 16), (1, 2)))
    w_out = centred(arg_keys[4], (D_ATT, D), D_ATT ** -0.5, 0.1875, ((0, 2), (1, 16)))
    return {"tokens": tokens, "w_query": w_query, "w_key": w_key, "w_value": w_value, "w_out": w_out}


dilation_rates = (1, 4, 16)
neg_big = -1e30


def band(query_class_rows, key_class_rows, value_class_rows, key_first_index):
    sequence_length = query_class_rows.shape[0]
    if sequence_length <= KEYS_BEHIND:
        blocks = 1
        step = sequence_length
        q_blk = query_class_rows[None]
        k_blk = key_class_rows[None]
        v_blk = value_class_rows[None]
    else:
        blocks = sequence_length // KEYS_BEHIND
        step = KEYS_BEHIND
        q_blk = query_class_rows.reshape(blocks, KEYS_BEHIND, HEAD_SIZE)
        k_rows = key_class_rows.reshape(blocks + 1, KEYS_BEHIND, HEAD_SIZE)
        v_rows = value_class_rows.reshape(blocks + 1, KEYS_BEHIND, HEAD_SIZE)
        k_blk = jnp.concatenate([k_rows[:-1], k_rows[1:]], axis=1)
        v_blk = jnp.concatenate([v_rows[:-1], v_rows[1:]], axis=1)
    score = jnp.einsum('nqd,nkd->nqk', q_blk.astype(jnp.float32), k_blk.astype(jnp.float32)) * (HEAD_SIZE ** -0.5)
    row_at = jnp.arange(step, dtype=jnp.int32)[:, None]
    col_at = jnp.arange(k_blk.shape[1], dtype=jnp.int32)[None, :]
    dist = KEYS_BEHIND + row_at - col_at
    key_pos = key_first_index + jnp.arange(blocks, dtype=jnp.int32)[:, None, None] * step + col_at[None]
    mask = (dist >= 0) & (dist <= KEYS_BEHIND) & (key_pos >= 0)
    score = jnp.where(mask, score, neg_big)
    top = jnp.max(score, axis=-1, keepdims=True)
    weight = jnp.exp(score - top)
    denom = jnp.sum(weight, axis=-1)
    weight_bf = weight.astype(jnp.bfloat16)
    out = jnp.einsum('nqk,nkd->nqd', weight_bf.astype(jnp.float32), v_blk.astype(jnp.float32)) / denom[..., None]
    lse = top[..., 0] + jnp.log(denom)
    return out.reshape(sequence_length, HEAD_SIZE), lse.reshape(sequence_length)


def one_head(parts):
    query_head_rows, key_head_rows, value_head_rows = parts
    outs = []
    lses = []
    for dilation_rate in dilation_rates:
        sequence_length = SEQUENCE_TOKENS // dilation_rate
        query_class_rows = query_head_rows.reshape(sequence_length, dilation_rate, HEAD_SIZE).transpose(1, 0, 2)
        padding_rows = jnp.zeros((KEYS_BEHIND * dilation_rate, HEAD_SIZE), jnp.bfloat16)
        key_class_rows = jnp.concatenate([padding_rows, key_head_rows], 0).reshape(KEYS_BEHIND + sequence_length, dilation_rate, HEAD_SIZE).transpose(1, 0, 2)
        value_class_rows = jnp.concatenate([padding_rows, value_head_rows], 0).reshape(KEYS_BEHIND + sequence_length, dilation_rate, HEAD_SIZE).transpose(1, 0, 2)
        out, lse = jax.vmap(lambda a, b, c: band(a, b, c, -KEYS_BEHIND))(query_class_rows, key_class_rows, value_class_rows)
        outs.append(out.transpose(1, 0, 2).reshape(SEQUENCE_TOKENS, HEAD_SIZE))
        lses.append(lse.T.reshape(SEQUENCE_TOKENS))
    lse_all = jnp.stack(lses, 0)
    peak = jnp.max(lse_all, axis=0)
    expo = jnp.exp(lse_all - peak)
    total = jnp.sum(expo, axis=0)
    mix = expo / total
    attended = jnp.sum(mix[..., None] * jnp.stack(outs, 0), axis=0)
    return attended, peak + jnp.log(total)


def reference(tokens, w_query, w_key, w_value, w_out):
    query_input = jnp.dot(tokens, w_query, preferred_element_type=jnp.float32).astype(jnp.bfloat16)
    keys = jnp.dot(tokens, w_key, preferred_element_type=jnp.float32).astype(jnp.bfloat16)
    values = jnp.dot(tokens, w_value, preferred_element_type=jnp.float32).astype(jnp.bfloat16)

    def heads_first(a):
        return a.reshape(SEQUENCE_TOKENS, HEADS, HEAD_SIZE).transpose(1, 0, 2)

    attended, row_lse = lax.map(one_head, (heads_first(query_input), heads_first(keys), heads_first(values)))
    attended = attended.transpose(1, 0, 2).reshape(SEQUENCE_TOKENS, D_ATT).astype(jnp.bfloat16)
    cols = D_ATT // N_TP
    total = jnp.zeros((SEQUENCE_TOKENS, D), jnp.float32)
    for group in range(N_TP):
        part = jnp.dot(attended[:, group * cols:(group + 1) * cols], w_out[group * cols:(group + 1) * cols],
                       preferred_element_type=jnp.float32).astype(jnp.bfloat16)
        total = total + part.astype(jnp.float32)
    return total.astype(jnp.bfloat16), row_lse
```

```python
from functools import partial

import jax
import jax.numpy as jnp
from jax import lax
from jax.experimental import pallas as pl
from jax.experimental.pallas import tpu as pltpu
from jax.sharding import PartitionSpec as P

HEAD_SIZE = 64
KEYS_BEHIND = 128
RATE = 16
CHUNK = RATE * RATE
NEG = -1e30


def swap_matrix():
    i = lax.broadcasted_iota(jnp.int32, (CHUNK, CHUNK), 0)
    j = lax.broadcasted_iota(jnp.int32, (CHUNK, CHUNK), 1)
    return jnp.where(j == (i % RATE) * RATE + i // RATE, 1.0, 0.0).astype(jnp.bfloat16)


def attention_kernel(where_ref, qkv_ref, prev_ref, att_ref, lse_ref, qs, ks, vs, b1, b4, b16, acc, top, den,
                     *, group, halves, width):
    group_at, half_at, plane = where_ref[0], where_ref[1], where_ref[2]
    heads = width // HEAD_SIZE
    chunks = qs.shape[0]
    held = ks.shape[0] - chunks
    per_block = chunks // group
    sub = per_block // halves
    swap = swap_matrix()
    lane = lax.broadcasted_iota(jnp.int32, (1, width), 1)

    def source(n):
        block = (n // per_block) ^ group_at
        half = (n % per_block) // sub
        half = jnp.where(block == 0, half, half ^ half_at)
        return (block * halves + half) * sub + n % sub

    def swapped(rows):
        return jnp.dot(swap, rows, preferred_element_type=jnp.float32)

    for n in range(chunks):
        x = swapped(qkv_ref[source(n)])
        qs[n] = (x[:, :width] * HEAD_SIZE ** -0.5).astype(jnp.bfloat16)
        ks[held + n] = x[:, width:2 * width].astype(jnp.bfloat16)
        vs[held + n] = x[:, 2 * width:].astype(jnp.bfloat16)
    planes = prev_ref.shape[0]
    skip = planes * chunks - held
    for n in range(held):
        x = swapped(prev_ref[(n + skip) // chunks, source((n + skip) % chunks)])
        ks[n] = x[:, :width].astype(jnp.bfloat16)
        vs[n] = x[:, width:].astype(jnp.bfloat16)

    def bias(ref, position_q, position_k):
        rows, cols = ref.shape[0] // heads, ref.shape[1]
        q = position_q(lax.broadcasted_iota(jnp.int32, (rows, cols), 0))
        k = position_k(lax.broadcasted_iota(jnp.int32, (rows, cols), 1))
        dist = q - k
        off = jnp.where((dist >= 0) & (dist <= KEYS_BEHIND), 0.0, NEG)
        for h in range(heads):
            ref[h * rows:(h + 1) * rows] = off

    bias(b16, lambda i: i + held * RATE, lambda j: j)
    bias(b4, lambda i: 4 * ((i // 64) * RATE + i % RATE) + (i % 64) // RATE + KEYS_BEHIND,
         lambda j: 4 * ((j // 64) * RATE + j % RATE) + (j % 64) // RATE)
    bias(b1, lambda i: RATE * (i % RATE) + i // RATE + CHUNK,
         lambda j: (j // CHUNK) * CHUNK + RATE * (j % RATE) + (j % CHUNK) // RATE)

    def absent(n):
        if n >= held:
            return None
        return jnp.where(plane * chunks + n - held >= 0, 0.0, NEG)

    def per_head(x, rows):
        if heads == 1:
            return jnp.broadcast_to(x, (rows, width))
        out = x[(heads - 1) * rows:]
        for h in reversed(range(heads - 1)):
            out = jnp.where(lane < (h + 1) * HEAD_SIZE, x[h * rows:(h + 1) * rows], out)
        return jnp.broadcast_to(out, (rows, width))

    def block(q, k, v, off):
        rows = q.shape[0]
        if heads > 1:
            zero = jnp.zeros_like(q)
            q = jnp.concatenate([jnp.where(lane // HEAD_SIZE == h, q, zero) for h in range(heads)], 0)
        score = lax.dot_general(q, k, (((1,), (1,)), ((), ())), preferred_element_type=jnp.float32) + off
        high = jnp.max(score, axis=-1, keepdims=True)
        weight = jnp.exp(score - high)
        total = jnp.sum(weight, axis=-1, keepdims=True)
        out = jnp.dot(weight.astype(jnp.bfloat16), v, preferred_element_type=jnp.float32)
        return per_head(out, rows), per_head(high, rows), per_head(total, rows)

    def merged(old, new):
        (o0, m0, l0), (o1, m1, l1) = old, new
        m = jnp.maximum(m0, m1)
        e0, e1 = jnp.exp(m0 - m), jnp.exp(m1 - m)
        return o0 * e0 + o1 * e1, m, l0 * e0 + l1 * e1

    def masked(ref, rows_per_chunk, where_chunks, rows=None):
        off = ref[...] if rows is None else ref[rows]
        gone = [absent(n) for n in where_chunks]
        if all(x is None for x in gone):
            return off
        col = lax.broadcasted_iota(jnp.int32, (1, off.shape[1]), 1) // rows_per_chunk
        add = jnp.zeros((1, off.shape[1]), jnp.float32)
        for at, x in enumerate(gone):
            if x is not None:
                add = jnp.where(col == at, x, add)
        return off + add

    def rows_of(ref, picks):
        return jnp.concatenate([ref[n, r * RATE:(r + 1) * RATE] for n, r in picks], 0)

    def put(picks, values):
        for at, (n, r) in enumerate(picks):
            for ref, x in zip((acc, top, den), values):
                ref[n, r * RATE:(r + 1) * RATE] = x[at * RATE:(at + 1) * RATE]

    off16 = masked(b16, RATE, range(held + chunks))
    for r in range(RATE):
        picks = [(n, r) for n in range(chunks)]
        keys = [(n, r) for n in range(held + chunks)]
        put(picks, block(rows_of(qs, picks), rows_of(ks, keys), rows_of(vs, keys), off16))

    for two in range(0, chunks, 2):
        off4 = masked(b4, 64, [held + two - 2, held + two - 1, held + two, held + two + 1])
        for c in range(4):
            picks = [(n, c + 4 * i) for n in (two, two + 1) for i in range(4)]
            keys = [(n, c + 4 * i) for n in range(held + two - 2, held + two + 2) for i in range(4)]
            new = block(rows_of(qs, picks), rows_of(ks, keys), rows_of(vs, keys), off4)
            put(picks, merged([rows_of(ref, picks) for ref in (acc, top, den)], new))

    part = CHUNK // 2
    for n in range(chunks):
        k = jnp.concatenate([ks[held + n - 1], ks[held + n]], 0)
        v = jnp.concatenate([vs[held + n - 1], vs[held + n]], 0)
        done, lses = [], []
        for p in range(2):
            rows = slice(p * part, (p + 1) * part)
            off = masked(b1, CHUNK, [held + n - 1, held + n])
            off = jnp.concatenate([off[h * CHUNK + p * part:h * CHUNK + (p + 1) * part] for h in range(heads)], 0)
            new = block(qs[n, rows], k, v, off)
            o, m, l = merged([ref[n, rows] for ref in (acc, top, den)], new)
            done.append((o / l).astype(jnp.bfloat16))
            lses.append(m + jnp.log(l))
        att_ref[n] = swapped(jnp.concatenate(done, 0)).astype(jnp.bfloat16)
        lse = jnp.concatenate(lses, 0).T
        for h in range(heads):
            lse_ref[h, n:n + 1] = lse[h * HEAD_SIZE:h * HEAD_SIZE + 1]


def attention(at, qkv, prev, group, halves):
    chunks, _, three = qkv.shape
    width = three // 3
    heads = width // HEAD_SIZE
    held = KEYS_BEHIND * RATE // CHUNK
    vmem = pl.BlockSpec(memory_space=pltpu.VMEM)
    return pl.pallas_call(
        partial(attention_kernel, group=group, halves=halves, width=width),
        in_specs=[pl.BlockSpec(memory_space=pltpu.SMEM), vmem, vmem],
        out_specs=[vmem, vmem],
        out_shape=[
            jax.ShapeDtypeStruct((chunks, CHUNK, width), jnp.bfloat16),
            jax.ShapeDtypeStruct((heads, chunks, CHUNK), jnp.float32),
        ],
        scratch_shapes=[
            pltpu.VMEM((chunks, CHUNK, width), jnp.bfloat16),
            pltpu.VMEM((held + chunks, CHUNK, width), jnp.bfloat16),
            pltpu.VMEM((held + chunks, CHUNK, width), jnp.bfloat16),
            pltpu.VMEM((heads * CHUNK, 2 * CHUNK), jnp.float32),
            pltpu.VMEM((heads * 128, 256), jnp.float32),
            pltpu.VMEM((heads * chunks * RATE, (held + chunks) * RATE), jnp.float32),
            pltpu.VMEM((chunks, CHUNK, width), jnp.float32),
            pltpu.VMEM((chunks, CHUNK, width), jnp.float32),
            pltpu.VMEM((chunks, CHUNK, width), jnp.float32),
        ],
        name="dilated",
    )(at, qkv, prev)


def natural(parts, at):
    parts = list(parts)
    bit = 1
    while bit < len(parts):
        flip = (at & bit) != 0
        parts = [jnp.where(flip, parts[j ^ bit], parts[j]) for j in range(len(parts))]
        bit *= 2
    return parts


def shards(tokens, w_query, w_key, w_value, w_out):
    rows, model = tokens.shape
    fan, width = w_query.shape
    devices, cores = lax.axis_size("sp"), lax.axis_size("tp")
    group = 4
    while width % (group * HEAD_SIZE) or devices % group:
        group //= 2
    planes = devices // group
    here, core = lax.axis_index("sp"), lax.axis_index("tp")
    group_at, plane = here % group, here // group
    cols = width // group
    heads = cols // HEAD_SIZE

    def across(x, step):
        return lax.ppermute(x, "sp", [(j, j ^ step) for j in range(devices)])

    def beyond(x, step):
        pairs = [(p * group + g, (p + step) * group + g) for p in range(planes - step) for g in range(group)]
        return lax.ppermute(x, "sp", pairs)

    def along(x):
        if planes > 8:
            lines = [[p * group + g for p in range(planes)] for g in range(group)]
            return lax.all_gather(x, "sp", axis=0, axis_index_groups=lines)
        out = jnp.zeros((planes + 1,) + x.shape, x.dtype)
        out = lax.dynamic_update_index_in_dim(out, x, plane, 0)
        up = down = x
        for s in range(1, planes):
            up_pairs = [(p, p + 1) for p in range(s - 1, planes - 1)]
            down_pairs = [(p, p - 1) for p in range(1, planes - s + 1)]
            up = lax.ppermute(up, "sp", [(p * group + g, q * group + g) for p, q in up_pairs for g in range(group)])
            down = lax.ppermute(down, "sp", [(p * group + g, q * group + g) for p, q in down_pairs for g in range(group)])
            out = lax.dynamic_update_index_in_dim(out, up, jnp.where(plane >= s, plane - s, planes), 0)
            out = lax.dynamic_update_index_in_dim(out, down, jnp.where(plane + s < planes, plane + s, planes), 0)
        return out[:planes]

    def gathered(x):
        if group == 1:
            return [[x]]
        one = across(x, 1)
        if group == 2:
            return [[x], [one]]
        two = across(x, 2)
        half = x.shape[0] // 2
        return [[x], [one], [two], [across(two[:half], 1), across(one[half:], 2)]]

    parts = jnp.concatenate([w.reshape(fan, group, cols) for w in (w_query, w_key, w_value)], 2).transpose(1, 0, 2)
    pieces = []
    for j in range(group):
        piece = lax.dynamic_index_in_dim(parts, group_at ^ j, 0, keepdims=False)
        pieces.append(across(piece, j) if j else piece)
    w_plane = jnp.concatenate(natural(pieces, group_at), 0)
    w_all = along(w_plane).reshape(model, 3 * cols)

    def project(x):
        return jnp.dot(x, w_all, preferred_element_type=jnp.float32).astype(jnp.bfloat16)

    share = rows // cores
    mine = lax.dynamic_slice_in_dim(tokens, core * share, share, 0)
    projected = [project(tokens)]
    for block in gathered(mine)[1:]:
        if cores == 2:
            projected += [project(x) for x in block]
            projected += [project(lax.ppermute(x, "tp", [(0, 1), (1, 0)])) for x in block]
        else:
            whole = lax.all_gather(jnp.concatenate(block, 0), "tp", axis=0, tiled=True)
            projected.append(project(whole))
    qkv = jnp.concatenate(projected, 0)
    halves = 2 if cores == 2 and group > 1 else 1
    half_at = core if halves == 2 else 0

    total = rows * group
    reach = (KEYS_BEHIND * RATE + total - 1) // total
    kv = qkv[:, cols:]
    prev = [beyond(kv, s) for s in range(reach, 0, -1)]
    prev = jnp.stack(prev, 0).reshape(reach, total // CHUNK, CHUNK, 2 * cols)

    w_line = along(w_out.T)
    w_blocks = [jnp.concatenate(b, 0).reshape(planes, -1, width) if len(b) > 1 else b[0].reshape(planes, -1, width)
                for b in gathered(w_line.reshape(-1, width))]
    w_rows = jnp.stack(natural(w_blocks, group_at), 1).reshape(model, width)

    at = jnp.stack([group_at, jnp.asarray(half_at, jnp.int32), plane]).astype(jnp.int32)
    attended, lse = attention(at, qkv.reshape(total // CHUNK, CHUNK, 3 * cols), prev, group, halves)
    attended = attended.reshape(group, rows, cols)
    lse = lse.reshape(heads, total // CHUNK, RATE, RATE).swapaxes(2, 3).reshape(heads, group, rows).swapaxes(0, 1)

    def traded(x):
        out = []
        for j in range(group):
            piece = lax.dynamic_index_in_dim(x, group_at ^ j, 0, keepdims=False)
            out.append(across(piece, j) if j else piece)
        return natural(out, group_at)

    att = jnp.concatenate(traded(attended), 1)
    row_lse = jnp.concatenate(traded(lse), 0)

    def partial_out(x):
        return lax.dot_general(x, w_rows, (((1,), (1,)), ((), ())), preferred_element_type=jnp.float32).astype(jnp.bfloat16)

    if cores == 2:
        other = partial_out(lax.dynamic_slice_in_dim(att, (1 - core) * share, share, 0))
        got = lax.ppermute(other, "tp", [(0, 1), (1, 0)])
        own = partial_out(lax.dynamic_slice_in_dim(att, core * share, share, 0))
        mixed = (own.astype(jnp.float32) + got.astype(jnp.float32)).astype(jnp.bfloat16)
    else:
        mixed = lax.psum_scatter(partial_out(att), "tp", scatter_dimension=0, tiled=True)
    return (mixed, row_lse)


def solution(mesh):
    placed = (P("sp", None), P("sp", "tp"), P("sp", "tp"), P("sp", "tp"), P("tp", "sp"))
    return jax.shard_map(
        shards,
        mesh=mesh,
        in_specs=placed,
        out_specs=(P(("sp", "tp"), None), P("tp", "sp")),
        check_vma=False,
    )
```

```python
from functools import partial

import jax
import jax.numpy as jnp
from jax import lax
from jax.experimental import pallas as pl
from jax.experimental.pallas import tpu as pltpu
from jax.sharding import PartitionSpec as P

HEAD_SIZE = 64
KEYS_BEHIND = 128
RATE = 16
CHUNK = RATE * RATE
NEG = -1e30


VMEM = pl.BlockSpec(memory_space=pltpu.VMEM)
SMEM = pl.BlockSpec(memory_space=pltpu.SMEM)


def natural(parts, at):
    parts = list(parts)
    bit = 1
    while bit < len(parts):
        flip = (at & bit) != 0
        parts = [jnp.where(flip, parts[j ^ bit], parts[j]) for j in range(len(parts))]
        bit *= 2
    return parts


def prep_kernel(where_ref, q_ref, k_ref, v_ref, *outs):
    group = len(outs)
    cols = q_ref.shape[1] // group
    for t, ref in enumerate((k_ref, v_ref, q_ref)):
        w = ref[...]
        parts = natural([w[:, b * cols:(b + 1) * cols] for b in range(group)], where_ref[0])
        for j in range(group):
            outs[j][:, t * cols:(t + 1) * cols] = parts[j]


def prep(at, w_query, w_key, w_value, group):
    fan, width = w_query.shape
    return pl.pallas_call(
        prep_kernel,
        in_specs=[SMEM, VMEM, VMEM, VMEM],
        out_specs=[VMEM] * group,
        out_shape=[jax.ShapeDtypeStruct((fan, 3 * width // group), jnp.bfloat16)] * group,
        name="prep",
    )(at, w_query, w_key, w_value)


def collect_kernel(where_ref, *refs):
    pieces, (kv_ref, q_ref) = refs[:-2], refs[-2:]
    fan, two = pieces[0].shape[0], kv_ref.shape[1]
    for j, ref in enumerate(pieces):
        at = pl.multiple_of((where_ref[0] ^ j) * fan, 16)
        kv_ref[pl.ds(at, fan), :] = ref[:, :two]
        q_ref[pl.ds(at, fan), :] = ref[:, two:]


def collect(at, pieces):
    fan, three = pieces[0].shape
    cols = three // 3
    shape = lambda n: jax.ShapeDtypeStruct((fan * len(pieces), n), jnp.bfloat16)
    return pl.pallas_call(
        collect_kernel,
        in_specs=[SMEM] + [VMEM] * len(pieces),
        out_specs=[VMEM, VMEM],
        out_shape=[shape(2 * cols), shape(cols)],
        name="collect",
    )(at, *pieces)


def weave_kernel(where_ref, *refs, plan, fan, group):
    pieces, out_ref = refs[:-1], refs[-1]
    cols = out_ref.shape[1] // group
    for ref, (j, first) in zip(pieces, plan):
        for p in range(ref.shape[0] // fan):
            w = ref[p * fan:(p + 1) * fan]
            parts = natural([w[:, b * cols:(b + 1) * cols] for b in range(group)], where_ref[0])
            to = pl.multiple_of(((first + p) * group + (where_ref[0] ^ j)) * fan, 16)
            for b in range(group):
                out_ref[pl.ds(to, fan), b * cols:(b + 1) * cols] = parts[b]


def weave(at, blocks, fan, group):
    plan, pieces = [], []
    for j, block in enumerate(blocks):
        first = 0
        for piece in block:
            plan.append((j, first))
            pieces.append(piece)
            first += piece.shape[0] // fan
    rows = sum(p.shape[0] for p in pieces)
    return pl.pallas_call(
        partial(weave_kernel, plan=plan, fan=fan, group=group),
        in_specs=[SMEM] + [VMEM] * len(pieces),
        out_specs=VMEM,
        out_shape=jax.ShapeDtypeStruct((rows, pieces[0].shape[1]), jnp.bfloat16),
        name="weave",
    )(at, *pieces)


def swap_matrix():
    i = lax.broadcasted_iota(jnp.int32, (CHUNK, CHUNK), 0)
    j = lax.broadcasted_iota(jnp.int32, (CHUNK, CHUNK), 1)
    return jnp.where(j == (i % RATE) * RATE + i // RATE, 1.0, 0.0).astype(jnp.bfloat16)


def attention_kernel(where_ref, *refs, group, width, layout, back, counts):
    n_q, n_kv, n_prev = counts
    q_refs, kv_refs, prev_refs = refs[:n_q], refs[n_q:n_q + n_kv], refs[n_q + n_kv:n_q + n_kv + n_prev]
    outs = refs[n_q + n_kv + n_prev:n_q + n_kv + n_prev + group]
    qs, ks, vs, b1, b4, b16, acc, top, den, done_at, lse_at = refs[n_q + n_kv + n_prev + group:]
    group_at, half_at, plane = where_ref[0], where_ref[1], where_ref[2]
    heads = width // HEAD_SIZE
    chunks = qs.shape[0]
    held = ks.shape[0] - chunks
    per_block = chunks // group
    swap = swap_matrix()
    lane = lax.broadcasted_iota(jnp.int32, (1, width), 1)

    def place(spot):
        j, half, sub, subs = spot
        inner = sub if half is None else (half_at ^ half) * subs + sub
        return (group_at ^ j) * per_block + inner

    def swapped(rows):
        return jnp.dot(swap, rows, preferred_element_type=jnp.float32)

    def rows_from(refs, pieces):
        got = [refs[i][first:first + size] for i, first, size in pieces]
        return got[0] if len(got) == 1 else jnp.concatenate(got, 0)

    for spot, pieces in layout:
        n = place(spot)
        qs[n] = (swapped(rows_from(q_refs, pieces)) * HEAD_SIZE ** -0.5).astype(jnp.bfloat16)
        x = swapped(rows_from(kv_refs, pieces))
        ks[held + n] = x[:, :width].astype(jnp.bfloat16)
        vs[held + n] = x[:, width:].astype(jnp.bfloat16)
    for step, spot, pieces in back:
        n = held - step * chunks + place(spot)
        x = swapped(rows_from(prev_refs, pieces))
        ks[n] = x[:, :width].astype(jnp.bfloat16)
        vs[n] = x[:, width:].astype(jnp.bfloat16)

    def bias(ref, position_q, position_k):
        rows, cols = ref.shape[0] // heads, ref.shape[1]
        q = position_q(lax.broadcasted_iota(jnp.int32, (rows, cols), 0))
        k = position_k(lax.broadcasted_iota(jnp.int32, (rows, cols), 1))
        dist = q - k
        off = jnp.where((dist >= 0) & (dist <= KEYS_BEHIND), 0.0, NEG)
        for h in range(heads):
            ref[h * rows:(h + 1) * rows] = off

    bias(b16, lambda i: i + held * RATE, lambda j: j)
    bias(b4, lambda i: 4 * ((i // 64) * RATE + i % RATE) + (i % 64) // RATE + KEYS_BEHIND,
         lambda j: 4 * ((j // 64) * RATE + j % RATE) + (j % 64) // RATE)
    bias(b1, lambda i: RATE * (i % RATE) + i // RATE + CHUNK,
         lambda j: (j // CHUNK) * CHUNK + RATE * (j % RATE) + (j % CHUNK) // RATE)

    def absent(n):
        if n >= held:
            return None
        return jnp.where(plane * chunks + n - held >= 0, 0.0, NEG)

    def per_head(x, rows):
        if heads == 1:
            return jnp.broadcast_to(x, (rows, width))
        out = x[(heads - 1) * rows:]
        for h in reversed(range(heads - 1)):
            out = jnp.where(lane < (h + 1) * HEAD_SIZE, x[h * rows:(h + 1) * rows], out)
        return jnp.broadcast_to(out, (rows, width))

    def block(q, k, v, off):
        rows = q.shape[0]
        if heads > 1:
            zero = jnp.zeros_like(q)
            q = jnp.concatenate([jnp.where(lane // HEAD_SIZE == h, q, zero) for h in range(heads)], 0)
        score = lax.dot_general(q, k, (((1,), (1,)), ((), ())), preferred_element_type=jnp.float32) + off
        high = jnp.max(score, axis=-1, keepdims=True)
        weight = jnp.exp(score - high)
        total = jnp.sum(weight, axis=-1, keepdims=True)
        out = jnp.dot(weight.astype(jnp.bfloat16), v, preferred_element_type=jnp.float32)
        return per_head(out, rows), per_head(high, rows), per_head(total, rows)

    def merged(old, new):
        (o0, m0, l0), (o1, m1, l1) = old, new
        m = jnp.maximum(m0, m1)
        e0, e1 = jnp.exp(m0 - m), jnp.exp(m1 - m)
        return o0 * e0 + o1 * e1, m, l0 * e0 + l1 * e1

    def masked(ref, rows_per_chunk, where_chunks):
        off = ref[...]
        gone = [absent(n) for n in where_chunks]
        if all(x is None for x in gone):
            return off
        col = lax.broadcasted_iota(jnp.int32, (1, off.shape[1]), 1) // rows_per_chunk
        add = jnp.zeros((1, off.shape[1]), jnp.float32)
        for at, x in enumerate(gone):
            if x is not None:
                add = jnp.where(col == at, x, add)
        return off + add

    def rows_of(ref, picks):
        return jnp.concatenate([ref[n, r * RATE:(r + 1) * RATE] for n, r in picks], 0)

    def put(picks, values):
        for at, (n, r) in enumerate(picks):
            for ref, x in zip((acc, top, den), values):
                ref[n, r * RATE:(r + 1) * RATE] = x[at * RATE:(at + 1) * RATE]

    off16 = masked(b16, RATE, range(held + chunks))
    for r in range(RATE):
        picks = [(n, r) for n in range(chunks)]
        keys = [(n, r) for n in range(held + chunks)]
        put(picks, block(rows_of(qs, picks), rows_of(ks, keys), rows_of(vs, keys), off16))

    for two in range(0, chunks, 2):
        off4 = masked(b4, 64, [held + two - 2, held + two - 1, held + two, held + two + 1])
        for c in range(4):
            picks = [(n, c + 4 * i) for n in (two, two + 1) for i in range(4)]
            keys = [(n, c + 4 * i) for n in range(held + two - 2, held + two + 2) for i in range(4)]
            new = block(rows_of(qs, picks), rows_of(ks, keys), rows_of(vs, keys), off4)
            put(picks, merged([rows_of(ref, picks) for ref in (acc, top, den)], new))

    part = CHUNK // 2
    for n in range(chunks):
        k = jnp.concatenate([ks[held + n - 1], ks[held + n]], 0)
        v = jnp.concatenate([vs[held + n - 1], vs[held + n]], 0)
        done, lses = [], []
        for p in range(2):
            rows = slice(p * part, (p + 1) * part)
            off = masked(b1, CHUNK, [held + n - 1, held + n])
            off = jnp.concatenate([off[h * CHUNK + p * part:h * CHUNK + (p + 1) * part] for h in range(heads)], 0)
            new = block(qs[n, rows], k, v, off)
            o, m, l = merged([ref[n, rows] for ref in (acc, top, den)], new)
            done.append((o / l).astype(jnp.bfloat16))
            lses.append(m + jnp.log(l))
        done_at[n] = swapped(jnp.concatenate(done, 0)).astype(jnp.bfloat16)
        lse = jnp.concatenate(lses, 0).T
        for h in range(heads):
            lse_at[n, h:h + 1] = lse[h * HEAD_SIZE:h * HEAD_SIZE + 1]

    for j, out in enumerate(outs):
        lines = []
        for c in range(per_block):
            n = (group_at ^ j) * per_block + c
            out[c * CHUNK:(c + 1) * CHUNK] = done_at[n]
            lse = lse_at[n]
            for h in range(heads):
                for at in range(0, CHUNK, width):
                    lines.append(lse[h:h + 1, at:at + width])
        size = -(-len(lines) // 16) * 16
        if size > len(lines):
            lines.append(jnp.zeros((size - len(lines), width), jnp.float32))
        rest = jnp.concatenate(lines, 0)
        for t in range(3):
            some = rest.astype(jnp.bfloat16)
            rest = rest - some.astype(jnp.float32)
            first = per_block * CHUNK + t * size
            out[first:first + size] = some


def lse_lines(rows, heads, width):
    used = rows * heads // width
    return used, -(-used // 16) * 16


def attention(at, qs, kvs, prevs, layout, back, group, rows):
    width = qs[0].shape[1]
    heads = width // HEAD_SIZE
    chunks = rows * group // CHUNK
    held = KEYS_BEHIND * RATE // CHUNK
    _, size = lse_lines(rows, heads, width)
    state = pltpu.VMEM((chunks, CHUNK, width), jnp.float32)
    own = pltpu.VMEM((chunks, CHUNK, width), jnp.bfloat16)
    both = pltpu.VMEM((held + chunks, CHUNK, width), jnp.bfloat16)
    return pl.pallas_call(
        partial(attention_kernel, group=group, width=width, layout=layout, back=back,
                counts=(len(qs), len(kvs), len(prevs))),
        in_specs=[SMEM] + [VMEM] * (len(qs) + len(kvs) + len(prevs)),
        out_specs=[VMEM] * group,
        out_shape=[jax.ShapeDtypeStruct((rows + 3 * size, width), jnp.bfloat16)] * group,
        scratch_shapes=[
            own, both, both,
            pltpu.VMEM((heads * CHUNK, 2 * CHUNK), jnp.float32),
            pltpu.VMEM((heads * 128, 256), jnp.float32),
            pltpu.VMEM((heads * chunks * RATE, (held + chunks) * RATE), jnp.float32),
            state, state, state, own,
            pltpu.VMEM((chunks, 8, CHUNK), jnp.float32),
        ],
        name="dilated",
    )(at, *qs, *kvs, *prevs)


def shards(tokens, w_query, w_key, w_value, w_out):
    rows, model = tokens.shape
    _, width = w_query.shape
    devices, cores = lax.axis_size("sp"), lax.axis_size("tp")
    group = 4
    while width % (group * HEAD_SIZE) or devices % group:
        group //= 2
    planes = devices // group
    here, core = lax.axis_index("sp"), lax.axis_index("tp")
    group_at, plane = here % group, here // group
    cols = width // group
    heads = cols // HEAD_SIZE
    split = cores == 2 and group > 1
    at = jnp.stack([group_at, core if split else 0 * core, plane]).astype(jnp.int32)

    def across(x, step):
        return lax.ppermute(x, "sp", [(j, j ^ step) for j in range(devices)])

    def beyond(x, step):
        pairs = [(p * group + g, (p + step) * group + g) for p in range(planes - step) for g in range(group)]
        return lax.ppermute(x, "sp", pairs)

    def swapped(x):
        return lax.ppermute(x, "tp", [(0, 1), (1, 0)])

    def along(x):
        if planes > 8:
            lines = [[p * group + g for p in range(planes)] for g in range(group)]
            return lax.all_gather(x, "sp", axis=0, axis_index_groups=lines)
        out = jnp.zeros((planes + 1,) + x.shape, x.dtype)
        out = lax.dynamic_update_index_in_dim(out, x, plane, 0)
        up = down = x
        for s in range(1, planes):
            up_pairs = [(p, p + 1) for p in range(s - 1, planes - 1)]
            down_pairs = [(p, p - 1) for p in range(1, planes - s + 1)]
            up = lax.ppermute(up, "sp", [(p * group + g, q * group + g) for p, q in up_pairs for g in range(group)])
            down = lax.ppermute(down, "sp", [(p * group + g, q * group + g) for p, q in down_pairs for g in range(group)])
            out = lax.dynamic_update_index_in_dim(out, up, jnp.where(plane >= s, plane - s, planes), 0)
            out = lax.dynamic_update_index_in_dim(out, down, jnp.where(plane + s < planes, plane + s, planes), 0)
        return out[:planes]

    def gathered(x):
        if group == 1:
            return [[x]]
        one = across(x, 1)
        if group == 2:
            return [[x], [one]]
        two = across(x, 2)
        half = x.shape[0] // 2
        return [[x], [one], [two], [across(two[:half], 1), across(one[half:], 2)]]

    pieces = prep(at, w_query, w_key, w_value, group)
    pieces = [pieces[0]] + [across(pieces[j], j) for j in range(1, group)]
    w_kv, w_q = collect(at, pieces)
    w_kv = along(w_kv).reshape(model, 2 * cols)
    w_q = along(w_q).reshape(model, cols)

    share = rows // cores
    mine = lax.dynamic_slice_in_dim(tokens, core * share, share, 0)
    held_rows = [[tokens]]
    for block in gathered(mine)[1:]:
        if split:
            held_rows.append(block + [swapped(x) for x in block])
        else:
            held_rows.append([lax.all_gather(jnp.concatenate(block, 0), "tp", axis=0, tiled=True)])

    layout, index = [], 0
    offsets = []
    for j, block in enumerate(held_rows):
        ends = []
        for i, piece in enumerate(block):
            ends += [(index + i, r) for r in range(0, piece.shape[0], 128)]
        for c in range(rows // CHUNK):
            marks = ends[2 * c:2 * c + 2]
            if marks[0][0] == marks[1][0]:
                got = [(marks[0][0], marks[0][1], CHUNK)]
            else:
                got = [(i, r, 128) for i, r in marks]
            subs = share // CHUNK
            spot = (j, c // subs, c % subs, subs) if split and j else (j, None, c, 0)
            layout.append((spot, got))
            offsets.append((j, c))
        index += len(block)

    flat = [x for block in held_rows for x in block]

    def project(x, w):
        return jnp.dot(x, w, preferred_element_type=jnp.float32).astype(jnp.bfloat16)

    kvs = [project(x, w_kv) for x in flat]
    qs = [project(x, w_q) for x in flat]

    early = sum(len(block) for block in held_rows[:max(group - 1, 1)])
    loads = [kvs[:early], kvs[early:]]
    loads = [jnp.concatenate(x, 0) if len(x) > 1 else x[0] for x in loads if x]
    reach = (KEYS_BEHIND * RATE + rows * group - 1) // (rows * group)
    prevs, back = [], []
    for s in range(reach, 0, -1):
        for (spot, _), (j, c) in zip(layout, offsets):
            late = j >= max(group - 1, 1)
            first = ((j - max(group - 1, 1)) if late else j) * rows + c * CHUNK
            back.append((s, spot, [(len(prevs) + int(late), first, CHUNK)]))
        prevs += [beyond(x, s) for x in loads]

    w_line = along(w_out.T).reshape(-1, width)
    w_rows = weave(at, gathered(w_line), w_out.shape[1], group)

    outs = attention(at, qs, kvs, prevs, layout, back, group, rows)
    outs = [outs[0]] + [across(outs[j], j) for j in range(1, group)]
    att = jnp.concatenate([x[:rows] for x in outs], 1)
    used, size = lse_lines(rows, heads, cols)

    def lse_of(x):
        x = sum(x[rows + t * size:rows + t * size + used].astype(jnp.float32) for t in range(3))
        x = x.reshape(rows // CHUNK, heads, RATE, RATE)
        return x.transpose(1, 0, 3, 2).reshape(heads, rows)

    row_lse = jnp.concatenate(natural([lse_of(x) for x in outs], group_at), 0)

    def partial_out(x):
        return lax.dot_general(x, w_rows, (((1,), (1,)), ((), ())), preferred_element_type=jnp.float32).astype(jnp.bfloat16)

    if cores == 2:
        other = partial_out(lax.dynamic_slice_in_dim(att, (1 - core) * share, share, 0))
        got = swapped(other)
        own = partial_out(lax.dynamic_slice_in_dim(att, core * share, share, 0))
        mixed = (own.astype(jnp.float32) + got.astype(jnp.float32)).astype(jnp.bfloat16)
    else:
        mixed = lax.psum_scatter(partial_out(att), "tp", scatter_dimension=0, tiled=True)
    return (mixed, row_lse)


def solution(mesh):
    placed = (P("sp", None), P("sp", "tp"), P("sp", "tp"), P("sp", "tp"), P("tp", "sp"))

    return jax.shard_map(
        shards,
        mesh=mesh,
        in_specs=placed,
        out_specs=(P(("sp", "tp"), None), P("tp", "sp")),
        check_vma=False,
    )
```

```python
from functools import partial

import jax
import jax.numpy as jnp
from jax import lax
from jax.experimental import pallas as pl
from jax.experimental.pallas import tpu as pltpu
from jax.sharding import PartitionSpec as P

HEAD_SIZE = 64
KEYS_BEHIND = 128
RATE = 16
CHUNK = RATE * RATE
NEG = -1e30


VMEM = pl.BlockSpec(memory_space=pltpu.VMEM)
SMEM = pl.BlockSpec(memory_space=pltpu.SMEM)


def natural(parts, at):
    parts = list(parts)
    bit = 1
    while bit < len(parts):
        flip = (at & bit) != 0
        parts = [jnp.where(flip, parts[j ^ bit], parts[j]) for j in range(len(parts))]
        bit *= 2
    return parts


def prep_kernel(where_ref, q_ref, k_ref, v_ref, *outs):
    group = len(outs)
    cols = q_ref.shape[1] // group
    for t, ref in enumerate((k_ref, v_ref, q_ref)):
        w = ref[...]
        parts = natural([w[:, b * cols:(b + 1) * cols] for b in range(group)], where_ref[0])
        for j in range(group):
            outs[j][:, t * cols:(t + 1) * cols] = parts[j]


def prep(at, w_query, w_key, w_value, group):
    fan, width = w_query.shape
    return pl.pallas_call(
        prep_kernel,
        in_specs=[SMEM, VMEM, VMEM, VMEM],
        out_specs=[VMEM] * group,
        out_shape=[jax.ShapeDtypeStruct((fan, 3 * width // group), jnp.bfloat16)] * group,
        name="prep",
    )(at, w_query, w_key, w_value)


def collect_kernel(where_ref, *refs):
    pieces, (kv_ref, q_ref) = refs[:-2], refs[-2:]
    fan, two = pieces[0].shape[0], kv_ref.shape[1]
    for j, ref in enumerate(pieces):
        at = pl.multiple_of((where_ref[0] ^ j) * fan, 16)
        kv_ref[pl.ds(at, fan), :] = ref[:, :two]
        q_ref[pl.ds(at, fan), :] = ref[:, two:]


def collect(at, pieces):
    fan, three = pieces[0].shape
    cols = three // 3
    shape = lambda n: jax.ShapeDtypeStruct((fan * len(pieces), n), jnp.bfloat16)
    return pl.pallas_call(
        collect_kernel,
        in_specs=[SMEM] + [VMEM] * len(pieces),
        out_specs=[VMEM, VMEM],
        out_shape=[shape(2 * cols), shape(cols)],
        name="collect",
    )(at, *pieces)


def line_kernel(where_ref, *refs):
    ins, out_ref = refs[:-1], refs[-1]
    plane, planes = where_ref[2], out_ref.shape[0]
    out_ref[plane] = ins[0][...]
    for s in range(1, planes):
        @pl.when(plane >= s)
        def _():
            out_ref[jnp.maximum(plane - s, 0)] = ins[2 * s - 1][...]

        @pl.when(plane + s < planes)
        def _():
            out_ref[jnp.minimum(plane + s, planes - 1)] = ins[2 * s][...]


def line(at, parts, planes):
    return pl.pallas_call(
        line_kernel,
        in_specs=[SMEM] + [VMEM] * len(parts),
        out_specs=VMEM,
        out_shape=jax.ShapeDtypeStruct((planes,) + parts[0].shape, jnp.bfloat16),
        name="line",
    )(at, *parts)


def weave_kernel(where_ref, *refs, plan, fan, group):
    pieces, out_ref = refs[:-1], refs[-1]
    cols = out_ref.shape[1] // group
    for ref, (j, first) in zip(pieces, plan):
        for p in range(ref.shape[0] // fan):
            w = ref[p * fan:(p + 1) * fan]
            parts = natural([w[:, b * cols:(b + 1) * cols] for b in range(group)], where_ref[0])
            to = pl.multiple_of(((first + p) * group + (where_ref[0] ^ j)) * fan, 16)
            for b in range(group):
                out_ref[pl.ds(to, fan), b * cols:(b + 1) * cols] = parts[b]


def weave(at, blocks, fan, group):
    plan, pieces = [], []
    for j, block in enumerate(blocks):
        first = 0
        for piece in block:
            plan.append((j, first))
            pieces.append(piece)
            first += piece.shape[0] // fan
    rows = sum(p.shape[0] for p in pieces)
    return pl.pallas_call(
        partial(weave_kernel, plan=plan, fan=fan, group=group),
        in_specs=[SMEM] + [VMEM] * len(pieces),
        out_specs=VMEM,
        out_shape=jax.ShapeDtypeStruct((rows, pieces[0].shape[1]), jnp.bfloat16),
        name="weave",
    )(at, *pieces)


def swap_matrix():
    i = lax.broadcasted_iota(jnp.int32, (CHUNK, CHUNK), 0)
    j = lax.broadcasted_iota(jnp.int32, (CHUNK, CHUNK), 1)
    return jnp.where(j == (i % RATE) * RATE + i // RATE, 1.0, 0.0).astype(jnp.bfloat16)


def attention_kernel(where_ref, *refs, group, width, layout, back, counts):
    n_q, n_kv, n_prev = counts
    q_refs, kv_refs, prev_refs = refs[:n_q], refs[n_q:n_q + n_kv], refs[n_q + n_kv:n_q + n_kv + n_prev]
    outs = refs[n_q + n_kv + n_prev:n_q + n_kv + n_prev + group]
    qs, ks, vs, b1, b4, b16, acc, top, den, done_at, lse_at = refs[n_q + n_kv + n_prev + group:]
    group_at, half_at, plane = where_ref[0], where_ref[1], where_ref[2]
    heads = width // HEAD_SIZE
    chunks = qs.shape[0]
    held = ks.shape[0] - chunks
    per_block = chunks // group
    swap = swap_matrix()
    lane = lax.broadcasted_iota(jnp.int32, (1, width), 1)

    def place(spot):
        j, half, sub, subs = spot
        inner = sub if half is None else (half_at ^ half) * subs + sub
        return (group_at ^ j) * per_block + inner

    def swapped(rows):
        return jnp.dot(swap, rows, preferred_element_type=jnp.float32)

    def rows_from(refs, pieces):
        got = [refs[i][first:first + size] for i, first, size in pieces]
        return got[0] if len(got) == 1 else jnp.concatenate(got, 0)

    for spot, pieces in layout:
        n = place(spot)
        qs[n] = (swapped(rows_from(q_refs, pieces)) * HEAD_SIZE ** -0.5).astype(jnp.bfloat16)
        x = swapped(rows_from(kv_refs, pieces))
        ks[held + n] = x[:, :width].astype(jnp.bfloat16)
        vs[held + n] = x[:, width:].astype(jnp.bfloat16)
    for step, spot, pieces in back:
        n = held - step * chunks + place(spot)
        x = swapped(rows_from(prev_refs, pieces))
        ks[n] = x[:, :width].astype(jnp.bfloat16)
        vs[n] = x[:, width:].astype(jnp.bfloat16)

    def bias(ref, position_q, position_k):
        rows, cols = ref.shape[0] // heads, ref.shape[1]
        q = position_q(lax.broadcasted_iota(jnp.int32, (rows, cols), 0))
        k = position_k(lax.broadcasted_iota(jnp.int32, (rows, cols), 1))
        dist = q - k
        off = jnp.where((dist >= 0) & (dist <= KEYS_BEHIND), 0.0, NEG)
        for h in range(heads):
            ref[h * rows:(h + 1) * rows] = off

    bias(b16, lambda i: i + held * RATE, lambda j: j)
    bias(b4, lambda i: 4 * ((i // 64) * RATE + i % RATE) + (i % 64) // RATE + KEYS_BEHIND,
         lambda j: 4 * ((j // 64) * RATE + j % RATE) + (j % 64) // RATE)
    bias(b1, lambda i: RATE * (i % RATE) + i // RATE + CHUNK,
         lambda j: (j // CHUNK) * CHUNK + RATE * (j % RATE) + (j % CHUNK) // RATE)

    def absent(n):
        if n >= held:
            return None
        return jnp.where(plane * chunks + n - held >= 0, 0.0, NEG)

    def per_head(x, rows):
        if heads == 1:
            return jnp.broadcast_to(x, (rows, width))
        out = x[(heads - 1) * rows:]
        for h in reversed(range(heads - 1)):
            out = jnp.where(lane < (h + 1) * HEAD_SIZE, x[h * rows:(h + 1) * rows], out)
        return jnp.broadcast_to(out, (rows, width))

    def block(q, k, v, off):
        rows = q.shape[0]
        if heads > 1:
            zero = jnp.zeros_like(q)
            q = jnp.concatenate([jnp.where(lane // HEAD_SIZE == h, q, zero) for h in range(heads)], 0)
        score = lax.dot_general(q, k, (((1,), (1,)), ((), ())), preferred_element_type=jnp.float32) + off
        high = jnp.max(score, axis=-1, keepdims=True)
        weight = jnp.exp(score - high)
        total = jnp.sum(weight, axis=-1, keepdims=True)
        out = jnp.dot(weight.astype(jnp.bfloat16), v, preferred_element_type=jnp.float32)
        return per_head(out, rows), per_head(high, rows), per_head(total, rows)

    def merged(old, new):
        (o0, m0, l0), (o1, m1, l1) = old, new
        m = jnp.maximum(m0, m1)
        e0, e1 = jnp.exp(m0 - m), jnp.exp(m1 - m)
        return o0 * e0 + o1 * e1, m, l0 * e0 + l1 * e1

    def masked(ref, rows_per_chunk, where_chunks):
        off = ref[...]
        gone = [absent(n) for n in where_chunks]
        if all(x is None for x in gone):
            return off
        col = lax.broadcasted_iota(jnp.int32, (1, off.shape[1]), 1) // rows_per_chunk
        add = jnp.zeros((1, off.shape[1]), jnp.float32)
        for at, x in enumerate(gone):
            if x is not None:
                add = jnp.where(col == at, x, add)
        return off + add

    def rows_of(ref, picks):
        return jnp.concatenate([ref[n, r * RATE:(r + 1) * RATE] for n, r in picks], 0)

    def put(picks, values):
        for at, (n, r) in enumerate(picks):
            for ref, x in zip((acc, top, den), values):
                ref[n, r * RATE:(r + 1) * RATE] = x[at * RATE:(at + 1) * RATE]

    off16 = masked(b16, RATE, range(held + chunks))
    for r in range(RATE):
        picks = [(n, r) for n in range(chunks)]
        keys = [(n, r) for n in range(held + chunks)]
        put(picks, block(rows_of(qs, picks), rows_of(ks, keys), rows_of(vs, keys), off16))

    for two in range(0, chunks, 2):
        off4 = masked(b4, 64, [held + two - 2, held + two - 1, held + two, held + two + 1])
        for c in range(4):
            picks = [(n, c + 4 * i) for n in (two, two + 1) for i in range(4)]
            keys = [(n, c + 4 * i) for n in range(held + two - 2, held + two + 2) for i in range(4)]
            new = block(rows_of(qs, picks), rows_of(ks, keys), rows_of(vs, keys), off4)
            put(picks, merged([rows_of(ref, picks) for ref in (acc, top, den)], new))

    part = CHUNK // 2
    for n in range(chunks):
        k = jnp.concatenate([ks[held + n - 1], ks[held + n]], 0)
        v = jnp.concatenate([vs[held + n - 1], vs[held + n]], 0)
        done, lses = [], []
        for p in range(2):
            rows = slice(p * part, (p + 1) * part)
            off = masked(b1, CHUNK, [held + n - 1, held + n])
            off = jnp.concatenate([off[h * CHUNK + p * part:h * CHUNK + (p + 1) * part] for h in range(heads)], 0)
            new = block(qs[n, rows], k, v, off)
            o, m, l = merged([ref[n, rows] for ref in (acc, top, den)], new)
            done.append((o / l).astype(jnp.bfloat16))
            lses.append(m + jnp.log(l))
        done_at[n] = swapped(jnp.concatenate(done, 0)).astype(jnp.bfloat16)
        lse = jnp.concatenate(lses, 0).T
        for h in range(heads):
            lse_at[n, h:h + 1] = lse[h * HEAD_SIZE:h * HEAD_SIZE + 1]

    for j, out in enumerate(outs):
        lines = []
        for c in range(per_block):
            n = (group_at ^ j) * per_block + c
            out[c * CHUNK:(c + 1) * CHUNK] = done_at[n]
            lse = lse_at[n]
            for h in range(heads):
                for at in range(0, CHUNK, width):
                    lines.append(lse[h:h + 1, at:at + width])
        size = -(-len(lines) // 16) * 16
        if size > len(lines):
            lines.append(jnp.zeros((size - len(lines), width), jnp.float32))
        rest = jnp.concatenate(lines, 0)
        for t in range(3):
            some = rest.astype(jnp.bfloat16)
            rest = rest - some.astype(jnp.float32)
            first = per_block * CHUNK + t * size
            out[first:first + size] = some


def lse_lines(rows, heads, width):
    used = rows * heads // width
    return used, -(-used // 16) * 16


def attention(at, qs, kvs, prevs, layout, back, group, rows):
    width = qs[0].shape[1]
    heads = width // HEAD_SIZE
    chunks = rows * group // CHUNK
    held = KEYS_BEHIND * RATE // CHUNK
    _, size = lse_lines(rows, heads, width)
    state = pltpu.VMEM((chunks, CHUNK, width), jnp.float32)
    own = pltpu.VMEM((chunks, CHUNK, width), jnp.bfloat16)
    both = pltpu.VMEM((held + chunks, CHUNK, width), jnp.bfloat16)
    return pl.pallas_call(
        partial(attention_kernel, group=group, width=width, layout=layout, back=back,
                counts=(len(qs), len(kvs), len(prevs))),
        in_specs=[SMEM] + [VMEM] * (len(qs) + len(kvs) + len(prevs)),
        out_specs=[VMEM] * group,
        out_shape=[jax.ShapeDtypeStruct((rows + 3 * size, width), jnp.bfloat16)] * group,
        scratch_shapes=[
            own, both, both,
            pltpu.VMEM((heads * CHUNK, 2 * CHUNK), jnp.float32),
            pltpu.VMEM((heads * 128, 256), jnp.float32),
            pltpu.VMEM((heads * chunks * RATE, (held + chunks) * RATE), jnp.float32),
            state, state, state, own,
            pltpu.VMEM((chunks, 8, CHUNK), jnp.float32),
        ],
        name="dilated",
    )(at, *qs, *kvs, *prevs)


def shards(tokens, w_query, w_key, w_value, w_out):
    rows, model = tokens.shape
    _, width = w_query.shape
    devices, cores = lax.axis_size("sp"), lax.axis_size("tp")
    group = 4
    while width % (group * HEAD_SIZE) or devices % group:
        group //= 2
    planes = devices // group
    here, core = lax.axis_index("sp"), lax.axis_index("tp")
    group_at, plane = here % group, here // group
    cols = width // group
    heads = cols // HEAD_SIZE
    split = cores == 2 and group > 1
    at = jnp.stack([group_at, core if split else 0 * core, plane]).astype(jnp.int32)

    def across(x, step):
        return lax.ppermute(x, "sp", [(j, j ^ step) for j in range(devices)])

    def beyond(x, step):
        pairs = [(p * group + g, (p + step) * group + g) for p in range(planes - step) for g in range(group)]
        return lax.ppermute(x, "sp", pairs)

    def swapped(x):
        return lax.ppermute(x, "tp", [(0, 1), (1, 0)])

    def along(x, eager):
        if planes > 8:
            lines = [[p * group + g for p in range(planes)] for g in range(group)]
            return lax.all_gather(x, "sp", axis=0, axis_index_groups=lines)
        out = None
        if eager:
            out = jnp.zeros((planes + 1,) + x.shape, x.dtype)
            out = lax.dynamic_update_index_in_dim(out, x, plane, 0)
        parts = [x]
        up = down = x
        for s in range(1, planes):
            up_pairs = [(p, p + 1) for p in range(s - 1, planes - 1)]
            down_pairs = [(p, p - 1) for p in range(1, planes - s + 1)]
            up = lax.ppermute(up, "sp", [(p * group + g, q * group + g) for p, q in up_pairs for g in range(group)])
            down = lax.ppermute(down, "sp", [(p * group + g, q * group + g) for p, q in down_pairs for g in range(group)])
            parts += [up, down]
            if eager:
                out = lax.dynamic_update_index_in_dim(out, up, jnp.where(plane >= s, plane - s, planes), 0)
                out = lax.dynamic_update_index_in_dim(out, down, jnp.where(plane + s < planes, plane + s, planes), 0)
        return out[:planes] if eager else parts

    def lined(parts, late):
        if planes > 8:
            return parts
        return line(lax.optimization_barrier((at, late))[0], parts, planes)

    def gathered(x, cut=None):
        if group == 1:
            return [[x]]
        one = across(x, 1)
        if group == 2:
            return [[x], [one]]
        two = across(x, 2)
        half = x.shape[0] // 2
        first, second = two[:half], one[half:]
        if cut is not None:
            cut += [first, second]
        return [[x], [one], [two], [across(first, 1), across(second, 2)]]

    pieces = prep(at, w_query, w_key, w_value, group)
    pieces = [pieces[0]] + [across(pieces[j], j) for j in range(1, group)]
    w_kv, w_q = collect(at, pieces)
    w_kv = along(w_kv, True).reshape(model, 2 * cols)
    q_parts = along(w_q, False)

    share = rows // cores
    mine = lax.dynamic_slice_in_dim(tokens, core * share, share, 0)
    held_rows = [[tokens]]
    passed = []
    gotten = gathered(mine, passed)
    w_kv = lax.optimization_barrier((w_kv, *passed))[0]
    for block in gotten[1:]:
        if split:
            held_rows.append(block + [swapped(x) for x in block])
        else:
            held_rows.append([lax.all_gather(jnp.concatenate(block, 0), "tp", axis=0, tiled=True)])

    layout, index = [], 0
    offsets = []
    for j, block in enumerate(held_rows):
        ends = []
        for i, piece in enumerate(block):
            ends += [(index + i, r) for r in range(0, piece.shape[0], 128)]
        for c in range(rows // CHUNK):
            marks = ends[2 * c:2 * c + 2]
            if marks[0][0] == marks[1][0]:
                got = [(marks[0][0], marks[0][1], CHUNK)]
            else:
                got = [(i, r, 128) for i, r in marks]
            subs = share // CHUNK
            spot = (j, c // subs, c % subs, subs) if split and j else (j, None, c, 0)
            layout.append((spot, got))
            offsets.append((j, c))
        index += len(block)

    flat = [x for block in held_rows for x in block]

    def project(x, w):
        return jnp.dot(x, w, preferred_element_type=jnp.float32).astype(jnp.bfloat16)

    early = sum(len(block) for block in held_rows[:max(group - 1, 1)])
    kvs = [project(x, w_kv) for x in flat[:early]]
    loads = [jnp.concatenate(kvs, 0)]
    if early < len(flat):
        flat[early:] = lax.optimization_barrier((*flat[early:], loads[0]))[:-1]
        kvs += [project(x, w_kv) for x in flat[early:]]
        loads.append(jnp.concatenate(kvs[early:], 0))
    w_q = lined(q_parts, loads[0]).reshape(model, cols)
    qs = [project(x, w_q) for x in flat]

    reach = (KEYS_BEHIND * RATE + rows * group - 1) // (rows * group)
    prevs, back = [], []
    for s in range(reach, 0, -1):
        for (spot, _), (j, c) in zip(layout, offsets):
            late = j >= max(group - 1, 1)
            first = ((j - max(group - 1, 1)) if late else j) * rows + c * CHUNK
            back.append((s, spot, [(len(prevs) + int(late), first, CHUNK)]))
        prevs += [beyond(x, s) for x in loads]

    w_line = lined(along(w_out.T, False), loads[0]).reshape(-1, width)
    w_rows = weave(at, gathered(w_line), w_out.shape[1], group)

    outs = attention(at, qs, kvs, prevs, layout, back, group, rows)
    outs = [outs[0]] + [across(outs[j], j) for j in range(1, group)]
    att = jnp.concatenate([x[:rows] for x in outs], 1)
    used, size = lse_lines(rows, heads, cols)

    def lse_of(x):
        x = sum(x[rows + t * size:rows + t * size + used].astype(jnp.float32) for t in range(3))
        x = x.reshape(rows // CHUNK, heads, RATE, RATE)
        return x.transpose(1, 0, 3, 2).reshape(heads, rows)

    row_lse = jnp.concatenate(natural([lse_of(x) for x in outs], group_at), 0)

    def partial_out(x):
        return lax.dot_general(x, w_rows, (((1,), (1,)), ((), ())), preferred_element_type=jnp.float32).astype(jnp.bfloat16)

    if cores == 2:
        other = partial_out(lax.dynamic_slice_in_dim(att, (1 - core) * share, share, 0))
        got = swapped(other)
        own = partial_out(lax.dynamic_slice_in_dim(att, core * share, share, 0))
        mixed = (own.astype(jnp.float32) + got.astype(jnp.float32)).astype(jnp.bfloat16)
    else:
        mixed = lax.psum_scatter(partial_out(att), "tp", scatter_dimension=0, tiled=True)
    return (mixed, row_lse)


def solution(mesh):
    placed = (P("sp", None), P("sp", "tp"), P("sp", "tp"), P("sp", "tp"), P("tp", "sp"))

    return jax.shard_map(
        shards,
        mesh=mesh,
        in_specs=placed,
        out_specs=(P(("sp", "tp"), None), P("tp", "sp")),
        check_vma=False,
    )
```
